256 devices in a mesh: sp: 16 (over y, x), tp: 16 (over z, core).
Axes of the slice: x: 4, y: 4, z: 8, core: 2. Of those that a mesh axis runs over, the one named last changes fastest.
Arguments:
- moe_input: bfloat16 [4096, 4096], P('sp', 'tp'), may hold values from -6 to 6
- out_gate: bfloat16 [4096, 4096], P('sp', 'tp'), may hold values from -6 to 6
- in_gate: bfloat16 [4096, 4096], P('sp', 'tp'), may hold values from -6 to 6
- values: bfloat16 [4096, 4096], P('sp', 'tp'), may hold values from -6 to 6
- conv_taps: float32 [3, 4096], P(None, 'tp'), may hold values from -3 to 3
- out_proj: bfloat16 [4096, 4096], P(None, 'tp'), may hold values from -0.09375 to 0.09375
- route_ids: int32 [4096, 2], P('sp'), may hold values from 0 to 15, all different within a row; in each aligned block of 256 rows (0 to 255, 256 to 511, ...) at most 48 rows name the same one
- route_gates: float32 [4096, 2], P('sp'), may hold values from 0.1 to 0.9
- expert_gate: bfloat16 [16, 4096, 2048], P('sp', None, 'tp'), may hold values from -0.09375 to 0.09375
- expert_up: bfloat16 [16, 4096, 2048], P('sp', None, 'tp'), may hold values from -0.09375 to 0.09375
- expert_down: bfloat16 [16, 2048, 4096], P('sp', 'tp'), may hold values from -0.125 to 0.125
- cotangent: bfloat16 [4096, 4096], P('sp', 'tp'), may hold values from -6 to 6
Outputs:
- grad_out_gate: bfloat16 [4096, 4096], P('sp', 'tp')
- grad_in_gate: bfloat16 [4096, 4096], P('sp', 'tp')
- grad_values: bfloat16 [4096, 4096], P('sp', 'tp')
- grad_out_proj: float32 [4096, 4096], P('sp', 'tp')
- grad_expert_gate: float32 [16, 4096, 2048], P('sp', None, 'tp')
- grad_expert_up: float32 [16, 4096, 2048], P('sp', None, 'tp')
- grad_expert_down: float32 [16, 2048, 4096], P('sp', 'tp')
The draws below stay inside these ranges and needn't reach their ends.
Inputs may be any that keep to these rules, and one draw needn't show every extreme that they name: `route_ids`: the 2 experts of a token differ. In the rows of one device no expert is named by more than 48 assignments, and in some device's rows some expert is named by exactly 48.
All inputs are finite; a program needn't handle non-finite values.
Results may differ from the reference program's by a relative error of at most 0.014.
Values may be sent and summed in bfloat16 or wider, within the bound.
No kernel may reach another device: no remote copies, remote signals or barrier semaphores. Data moves between devices by JAX's collectives and lax.ppermute only.
A program may use at most 128 MiB of HBM per device.

```python
import math
import jax
import jax.numpy as jnp
import numpy as np
from jax import lax

D = 4096
C = 4096
F = 2048
TOP = 2
TOK = 256
EXPERTS = 16
CAP = 48
TOKENS = 4096
N_SP = 16


def strengthened(drawn, rng, source, target, blocks, factor):
    def block_of(dim):
        return (jnp.arange(drawn.shape[dim]) // (drawn.shape[dim] // blocks)).reshape((-1,) + (1,) * (drawn.ndim - 1 - dim))

    one_side = jax.random.permutation(rng, blocks)[block_of(target)]
    far = (block_of(target) + blocks // 2) % blocks
    return jnp.where((block_of(source) == one_side) | (block_of(source) == far), factor * drawn, drawn)


def steps_of(stream_key, shape, pieces, low, high):
    gain = 1.0
    for dim, parts in pieces:
        steps = jax.random.uniform(jax.random.fold_in(jax.random.fold_in(stream_key, 6), dim), (parts,), jnp.float32, low / len(pieces), high / len(pieces))
        gain = gain * jnp.repeat(jnp.exp(steps), shape[dim] // parts).reshape((-1,) + (1,) * (len(shape) - 1 - dim))
    return gain


def deal_out(key, own, number, rows, number_of, top, bound, slope):
    order = jax.random.permutation(key, number_of)
    crowded, common = load_shares(number_of, rows * top, bound, slope, True), load_shares(number_of, rows * top, bound, slope, False)
    places = jnp.arange(number_of)

    def named(sizes, turn):
        used = int((sizes > 0).sum())
        fixed = max(1, used // 4)
        moved = fixed + (places - fixed + turn * (used - fixed)) % max(1, number_of - fixed)
        return jnp.zeros((number_of,), jnp.int32).at[order[jnp.where(places < fixed, places, moved)]].set(jnp.asarray(sizes, jnp.int32))

    sizes = jnp.where(number % 4 == 0, named(crowded, number // 4), named(common, number - number // 4 - 1))
    mixed = jax.random.permutation(jax.random.fold_in(own, 3), number_of)
    source_of, receiver = mixed[0:number_of // 2 * 2:2], mixed[1:number_of // 2 * 2:2]
    margin = jnp.minimum(sizes[source_of] - 1, bound - sizes[receiver]) // 2
    margin = jnp.where((source_of == order[0]) | (receiver == order[0]) | (sizes[receiver] == 0), 0, jnp.maximum(margin, 0))
    moved = jax.random.randint(jax.random.fold_in(own, 4), (number_of // 2,), 0, 1 << 20) % (margin + 1)
    sizes = sizes.at[source_of].add(-moved).at[receiver].add(moved)
    items = jnp.searchsorted(jnp.cumsum(sizes), jnp.arange(rows * top), side="right").astype(jnp.int32)
    table = items.reshape(top, rows).T
    table = table[jax.random.permutation(jax.random.fold_in(own, 1), rows)]
    turn = jax.random.randint(jax.random.fold_in(own, 2), (rows, 1), 0, top)
    return jnp.take_along_axis(table, (jnp.arange(top)[None, :] + turn) % top, axis=1)


def load_shares(amount, total, bound, skew, full):
    loads = [(1 << 20) // math.isqrt(standing ** skew) + 1 for standing in range(1, amount + 1)]
    largest = bound if full else min(bound, max(-(-total // amount), total * loads[0] // sum(loads)))
    least = 1 if total - largest >= amount - 1 else 0
    holding, rest = [largest] + [least] * (amount - 1), total - largest - least * (amount - 1)
    while rest > 0:
        free = [i for i in range(1, amount) if holding[i] < largest] or [i for i in range(1, amount) if holding[i] < bound]
        whole, remaining = sum([loads[i] for i in free]), rest
        for i in free:
            addition = min(bound - holding[i], max(1, remaining * loads[i] // whole), rest)
            holding[i] = holding[i] + addition
            rest = rest - addition
    return np.array(holding)


def bell_draw(stream_key, shape, spread, most, cuts=(), kind=jnp.bfloat16):
    entries = spread * jax.random.normal(stream_key, shape, jnp.float32)
    if cuts:
        entries = entries * steps_of(stream_key, shape, cuts, -0.22, 0.18)
    return jnp.clip(entries, -most, most).astype(kind)


def gaussian_with(own_key, shape, scale, bound, split, heavy, kind=jnp.bfloat16):
    result = scale * jax.random.normal(own_key, shape, jnp.float32)
    if split:
        result = result * steps_of(own_key, shape, split, -0.22, 0.18)
    return jnp.clip(strengthened(result, jax.random.fold_in(own_key, 3), *heavy), -bound, bound).astype(kind)


def setup_inputs(seed: int = 0) -> dict:
    key_list = jax.random.split(jax.random.key(seed), 13)
    moe_input = bell_draw(key_list[0], (TOKENS, D), 1.0, 6.0, ((0, 16), (1, 16)))
    out_gate = bell_draw(key_list[1], (TOKENS, C), 1.0, 6.0, ((0, 16), (1, 16)))
    in_gate = bell_draw(key_list[2], (TOKENS, C), 1.0, 6.0, ((0, 16), (1, 16)))
    values = bell_draw(key_list[3], (TOKENS, C), 1.0, 6.0, ((0, 16), (1, 16)))
    conv_taps = bell_draw(key_list[4], (3, C), 0.5, 3.0, ((1, 16),), jnp.float32)
    out_proj = bell_draw(key_list[5], (D, C), C ** -0.5, 0.09375, ((1, 16),))
    route_ids_keys = jax.random.split(jax.random.fold_in(key_list[6], 1), TOKENS // TOK)
    route_ids_turns = jax.random.permutation(jax.random.fold_in(key_list[6], 3), TOKENS // TOK)
    route_ids = jax.vmap(lambda own, number: deal_out(jax.random.fold_in(key_list[6], 2), own, number, TOK, EXPERTS, TOP, CAP, 1))(route_ids_keys, route_ids_turns).reshape((TOKENS, TOP))
    route_gates = jnp.clip(0.1 + 0.79999997 * jax.random.uniform(key_list[7], (TOKENS, TOP), jnp.float32) ** steps_of(key_list[7], (TOKENS, TOP), ((0, 16),), -0.2, 0.2), 0.1, 0.9)
    expert_gate = bell_draw(key_list[8], (EXPERTS, D, F), D ** -0.5, 0.09375, ((0, 16), (2, 16)))
    expert_up = bell_draw(key_list[9], (EXPERTS, D, F), D ** -0.5, 0.09375, ((0, 16), (2, 16)))
    expert_down = bell_draw(key_list[10], (EXPERTS, F, D), F ** -0.5, 0.125, ((0, 16), (1, 16)))
    cotangent = gaussian_with(key_list[11], (TOKENS, D), 1.0, 6.0, ((0, 16), (1, 16)), (0, 1, 16, 2.0))
    return {"moe_input": moe_input, "out_gate": out_gate, "in_gate": in_gate, "values": values, "conv_taps": conv_taps, "out_proj": out_proj, "route_ids": route_ids, "route_gates": route_gates, "expert_gate": expert_gate, "expert_up": expert_up, "expert_down": expert_down, "cotangent": cotangent}


def reference(moe_input, out_gate, in_gate, values, conv_taps, out_proj, route_ids, route_gates, expert_gate, expert_up, expert_down, cotangent):
    slots = N_SP * CAP
    flat_ids = route_ids.reshape(-1)
    owner = jnp.arange(TOKENS * TOP, dtype=jnp.int32) // TOP
    one_hot = (flat_ids[:, None] == jnp.arange(EXPERTS, dtype=jnp.int32)[None, :]).astype(jnp.int32)
    blocked = one_hot.reshape(N_SP, TOK * TOP, EXPERTS)
    earlier = (jnp.cumsum(blocked, axis=1) - blocked).reshape(TOKENS * TOP, EXPERTS)
    position = jnp.sum(earlier * one_hot, axis=1).astype(jnp.int32)
    slot_index = (flat_ids * slots + (owner // TOK) * CAP + position).astype(jnp.int32)
    slot_token = jnp.full((EXPERTS * slots,), TOKENS, jnp.int32).at[slot_index].set(owner)
    slot_weight = jnp.zeros((EXPERTS * slots,), jnp.float32).at[slot_index].set(route_gates.reshape(-1))
    padded_input = jnp.concatenate([moe_input, jnp.zeros((1, D), moe_input.dtype)], axis=0)
    padded_cot = jnp.concatenate([cotangent, jnp.zeros((1, D), cotangent.dtype)], axis=0)
    contract_rows = (((0,), (0,)), ((), ()))
    contract_cols = (((1,), (1,)), ((), ()))

    def expert_backward(args):
        tokens_of, weights_of, gate_w, up_w, down_w = args
        rows = padded_input[tokens_of]
        routed = (weights_of[:, None] * padded_cot[tokens_of].astype(jnp.float32)).astype(jnp.bfloat16)
        pre_gate = jnp.dot(rows, gate_w, preferred_element_type=jnp.float32)
        pre_up = jnp.dot(rows, up_w, preferred_element_type=jnp.float32)
        gate_sig = jax.nn.sigmoid(pre_gate)
        activated = pre_gate * gate_sig
        hidden_act = (activated * pre_up).astype(jnp.bfloat16)
        grad_down = lax.dot_general(hidden_act, routed, contract_rows, preferred_element_type=jnp.float32)
        grad_hidden = lax.dot_general(routed, down_w, contract_cols, preferred_element_type=jnp.float32)
        grad_pre_gate = (grad_hidden * pre_up * gate_sig * (1.0 + pre_gate * (1.0 - gate_sig))).astype(jnp.bfloat16)
        grad_pre_up = (grad_hidden * activated).astype(jnp.bfloat16)
        grad_gate = lax.dot_general(rows, grad_pre_gate, contract_rows, preferred_element_type=jnp.float32)
        grad_up = lax.dot_general(rows, grad_pre_up, contract_rows, preferred_element_type=jnp.float32)
        assign = (lax.dot_general(grad_pre_gate, gate_w, contract_cols, preferred_element_type=jnp.float32)
                  + lax.dot_general(grad_pre_up, up_w, contract_cols, preferred_element_type=jnp.float32))
        return grad_gate, grad_up, grad_down, assign

    grad_expert_gate, grad_expert_up, grad_expert_down, assign = lax.map(
        expert_backward,
        (slot_token.reshape(EXPERTS, slots), slot_weight.reshape(EXPERTS, slots), expert_gate, expert_up, expert_down))
    flat_assign = assign.reshape(EXPERTS * slots, D)
    moe_grad = jnp.sum(flat_assign[slot_index].reshape(TOKENS, TOP, D), axis=1)
    mixer_cot = (cotangent.astype(jnp.float32) + moe_grad).astype(jnp.bfloat16)

    conv_in = in_gate.astype(jnp.float32) * values.astype(jnp.float32)
    rimmed = jnp.pad(conv_in, ((1, 1), (0, 0)))
    conv_out = rimmed[:-2] * conv_taps[0] + rimmed[1:-1] * conv_taps[1] + rimmed[2:] * conv_taps[2]
    mixed = (out_gate.astype(jnp.float32) * conv_out).astype(jnp.bfloat16)
    grad_mixed = jnp.dot(mixer_cot, out_proj, preferred_element_type=jnp.float32)
    grad_out_gate = (grad_mixed * conv_out).astype(jnp.bfloat16)
    grad_conv_out = grad_mixed * out_gate.astype(jnp.float32)
    rim_grad = jnp.pad(grad_conv_out, ((1, 1), (0, 0)))
    grad_conv_in = rim_grad[2:] * conv_taps[0] + rim_grad[1:-1] * conv_taps[1] + rim_grad[:-2] * conv_taps[2]
    grad_in_gate = (grad_conv_in * values.astype(jnp.float32)).astype(jnp.bfloat16)
    grad_values = (grad_conv_in * in_gate.astype(jnp.float32)).astype(jnp.bfloat16)
    grad_out_proj = lax.dot_general(mixer_cot, mixed, contract_rows, preferred_element_type=jnp.float32)
    return (grad_out_gate, grad_in_gate, grad_values, grad_out_proj, grad_expert_gate, grad_expert_up, grad_expert_down)
```

```python
import functools

import jax
import jax.numpy as jnp
from jax import lax
from jax.experimental import pallas as pl
from jax.experimental.pallas import tpu as pltpu
from jax.sharding import Mesh
from jax.sharding import PartitionSpec as P


BF = jnp.bfloat16
F32 = jnp.float32
NZ = 8
ZC = ("z", "c")
STEPS = (0, -1, -2, -3, -4, 1, 2, 3)
CORE_SWAP = [(0, 1), (1, 0)]


def tied(*arrays):
    return lax.optimization_barrier(arrays)


def along(sign):
    return [(z * 2 + c, (z + sign * (1 - 2 * c)) % NZ * 2 + c) for z in range(NZ) for c in range(2)]


def ring_gather(block, fill=None):
    blocks = {0: block}
    for k in range(1, 5):
        blocks[-k] = lax.ppermute(blocks[1 - k], ZC, along(1))
        keys = [-k]
        if k < 4:
            blocks[k] = lax.ppermute(blocks[k - 1], ZC, along(-1))
            keys.append(k)
        extra = fill(k, blocks) if fill else {}
        if k < 4:
            done = tied(*(blocks[j] for j in keys), *extra.values())
            blocks.update(zip(keys, done))
            extra.update(zip(extra, done[len(keys) :]))
    return blocks


def core_swap(array):
    return lax.ppermute(array, "c", CORE_SWAP)


def add_rounded(a, b):
    return (a.astype(F32) + b.astype(F32)).astype(BF)


def ring_scatter(chunks):
    ups = [parts[4] for parts in chunks]
    downs = [parts[-3] for parts in chunks]
    for k in range(3, -1, -1):
        for i, parts in enumerate(chunks):
            ups[i] = lax.ppermute(ups[i], ZC, along(1))
            if k < 3:
                downs[i] = lax.ppermute(downs[i], ZC, along(-1))
            if k:
                ups[i] = add_rounded(ups[i], parts[k])
                if k < 3:
                    downs[i] = add_rounded(downs[i], parts[-k])
                ups[i], downs[i] = tied(ups[i], downs[i])
    return [p[0].astype(F32) + u.astype(F32) + d.astype(F32) for p, u, d in zip(chunks, ups, downs)]


def block_ids():
    z, c = lax.axis_index("z"), lax.axis_index("c")
    sgn = 1 - 2 * c
    own = [(z + sgn * j + NZ) % NZ * 2 + c for j in STEPS]
    other = [(z - sgn * j + NZ) % NZ * 2 + (1 - c) for j in STEPS]
    return jnp.stack(own + other).astype(jnp.int32)


def call(kernel, ids, args, outs, flops):
    vmem = pl.BlockSpec(memory_space=pltpu.VMEM)
    return pl.pallas_call(
        kernel,
        in_specs=[pl.BlockSpec(memory_space=pltpu.SMEM)] + [vmem] * len(args),
        out_specs=[vmem] * len(outs),
        out_shape=outs,
        cost_estimate=pl.CostEstimate(flops=flops, bytes_accessed=flops // 500, transcendentals=0),
    )(ids, *args)


def dot(a, b, ca, cb):
    return lax.dot_general(a, b, (((ca,), (cb,)), ((), ())), preferred_element_type=F32)


def rows_of(ids, i, width):
    return pl.ds(pl.multiple_of(ids[i] * width, width), width)


def forward_kernel(ids, *refs):
    xs, (wg, wu, pre_gate, pre_up) = refs[:16], refs[16:]
    total = None
    for i, x in enumerate(xs):
        at = rows_of(ids, i, x.shape[1])
        w = jnp.concatenate([wg[at, :], wu[at, :]], axis=1)
        part = dot(x[...], w, 1, 0)
        total = part if total is None else total + part
    f = wg.shape[1]
    pre_gate[...] = total[:, :f]
    pre_up[...] = total[:, f:]


def hidden_kernel(ids, cot, wd, od, mine, theirs):
    width = cot.shape[1] // NZ
    f = wd.shape[0]
    total = None
    for i in range(NZ):
        at = rows_of(ids, i, width)
        w = jnp.concatenate([wd[:, at], od[:, at]], axis=0)
        part = dot(cot[:, i * width : (i + 1) * width], w, 1, 1)
        total = part if total is None else total + part
    mine[...] = total[:, :f]
    theirs[...] = total[:, f:]


def grads_kernel(ids, mine, theirs, pre_gate, pre_up, hact, gcat):
    total = mine[...] + theirs[...]
    gate, up = pre_gate[...], pre_up[...]
    sig = jax.nn.sigmoid(gate)
    act = gate * sig
    hact[...] = (act * up).astype(BF)
    f = gate.shape[1]
    gcat[:, :f] = (total * up * sig * (1.0 + gate * (1.0 - sig))).astype(BF)
    gcat[:, f:] = (total * act).astype(BF)


def partial_kernel(ids, gcat, gother, wg, wu, og, ou, *parts):
    g, h = gcat[...], gother[...]
    half = parts[0].shape[1]
    width = 2 * half
    for i in range(NZ):
        at = rows_of(ids, i, width)
        mine = jnp.concatenate([wg[at, :], wu[at, :]], axis=1)
        theirs = jnp.concatenate([og[at, :], ou[at, :]], axis=1)
        both = (dot(g, mine, 1, 1) + dot(h, theirs, 1, 1)).astype(BF)
        parts[2 * i][...] = both[:, :half]
        parts[2 * i + 1][...] = both[:, half:]


def weight_kernel(ids, *refs):
    xs, (own, other, gcat, hact, gg, gu, gd) = refs[:16], refs[16:]
    g, h = gcat[...], hact[...]
    f = gg.shape[1]
    for i, x in enumerate(xs):
        width = x.shape[1]
        at = rows_of(ids, i, width)
        both = dot(x[...], g, 0, 0)
        gg[at, :] = both[:, :f]
        gu[at, :] = both[:, f:]
        ref = own if i < NZ else other
        j = i % NZ
        gd[:, at] = dot(h, ref[:, j * width : (j + 1) * width], 0, 0)


def columns_kernel(ids, *refs):
    ms, cols = refs[:16], refs[16]
    half = cols.shape[1]
    first = pl.ds(pl.multiple_of(lax.rem(ids[0], 2) * half, half), half)
    for i, m in enumerate(ms):
        cols[ids[i]] = m[first, :]


def mixed_kernel(ids, *refs):
    ms, (proj, conv_out, out_gate, gog, gco) = refs[:16], refs[16:]
    total = None
    for i, m in enumerate(ms):
        part = dot(m[...], proj[rows_of(ids, i, m.shape[1]), :], 1, 0)
        total = part if total is None else total + part
    gog[...] = (total * conv_out[...]).astype(BF)
    gco[...] = total * out_gate[...].astype(F32)


def proj_kernel(ids, own, other, mixed, out):
    groups, half, width = own.shape

    def part(cols, at):
        rows = mixed[:, at : at + half, :]
        flat = (groups * half, width)
        return dot(cols[...].reshape(flat), rows.reshape(flat), 0, 0)

    out[...] = part(own, 0) + part(other, half)


def neighbours(first, last):
    size = lax.axis_size("sp")
    up = [(i, i + 1) for i in range(size - 1)]
    return lax.ppermute(last, "sp", up), lax.ppermute(first, "sp", [(j, i) for i, j in up])


def shifted(array, before, after):
    return jnp.concatenate([before, array[:-1]], axis=0), jnp.concatenate([array[1:], after], axis=0)


def sds(shape, dtype):
    return jax.ShapeDtypeStruct(shape, dtype)


def body(
    moe_input,
    out_gate,
    in_gate,
    values,
    conv_taps,
    out_proj,
    route_ids,
    route_gates,
    expert_gate,
    expert_up,
    expert_down,
    cotangent,
):
    tok, blk = moe_input.shape
    experts = lax.axis_size("sp")
    cap = 3 * tok // experts
    slots = experts * cap
    sp = lax.axis_index("sp")
    c = lax.axis_index("c")
    ids = block_ids()
    wg, wu, wd = expert_gate[0], expert_up[0], expert_down[0]
    depth, f = wg.shape

    with jax.named_scope("cot_gather"):
        cot_blocks = ring_gather(cotangent)

    ids_t = route_ids.T
    gates_t = route_gates.T
    which = jnp.arange(experts, dtype=jnp.int32)[:, None]
    hit = [ids_t[k][None, :] == which for k in range(ids_t.shape[0])]
    chosen = functools.reduce(jnp.logical_or, hit)
    weight = sum(jnp.where(h, gates_t[k][None, :], 0.0) for k, h in enumerate(hit))
    t = jnp.arange(tok, dtype=jnp.int32)
    before = (t[:, None] < t[None, :]).astype(BF)
    position = jnp.dot(chosen.astype(BF), before, preferred_element_type=F32).astype(jnp.int32)
    place = jnp.where(chosen, position, -1)
    pick = place[:, None, :] == jnp.arange(cap, dtype=jnp.int32)[None, :, None]
    select = pick.astype(BF).reshape(slots, tok)
    slot_weight = jnp.sum(jnp.where(pick, weight[:, None, :], 0.0), axis=2).reshape(slots, 1)

    send_x = jnp.dot(select, moe_input, preferred_element_type=F32).astype(BF)
    with jax.named_scope("x_send"):
        x0 = lax.all_to_all(send_x.reshape(experts, cap, blk), "sp", 0, 0, tiled=True)
        x0 = x0.reshape(slots, blk)
    cot_tokens = jnp.concatenate([cot_blocks[j] for j in STEPS], axis=1)
    send_c = (
        slot_weight * jnp.dot(select, cot_tokens, preferred_element_type=F32)
    ).astype(BF)

    conv_in = in_gate.astype(F32) * values.astype(F32)
    swapped = {}

    x_own = {0: x0}
    for k in range(1, 5):
        x_own[-k] = lax.ppermute(x_own[1 - k], ZC, along(1))
        if k < 4:
            x_own[k] = lax.ppermute(x_own[k - 1], ZC, along(-1))
        if k == 1:
            x_own[-1], x_own[1], send_c = tied(x_own[-1], x_own[1], send_c)
            own_cot = lax.all_to_all(
                send_c.reshape(experts, cap, NZ * blk), "sp", 0, 0, tiled=True
            ).reshape(slots, NZ * blk)
            swapped[0] = core_swap(x0)
            og, ou, od = (core_swap(w) for w in (wg, wu, wd))
        if k == 2:
            for j in (-1, 1):
                swapped[j] = core_swap(x_own[j])
            done = tied(x_own[-2], x_own[2], swapped[0], swapped[-1], swapped[1], og, ou, od, conv_in)
            x_own[-2], x_own[2], swapped[0], swapped[-1], swapped[1], og, ou, od, conv_in = done
            conv_ends = neighbours(conv_in[:1], conv_in[-1:])
        if k == 3:
            for j in (-2, 2):
                swapped[j] = core_swap(x_own[j])
            done = tied(x_own[-3], x_own[3], swapped[-2], swapped[2])
            x_own[-3], x_own[3], swapped[-2], swapped[2] = done
            for j in (-3, 3):
                swapped[j] = core_swap(x_own[j])
    swapped[-4] = core_swap(x_own[-4])
    xs = [x_own[j] for j in STEPS] + [swapped[j] for j in STEPS]
    own_cot, *conv_ends = tied(own_cot, *conv_ends)
    prev, nxt = shifted(conv_in, *conv_ends)
    conv_out = prev * conv_taps[0] + conv_in * conv_taps[1] + nxt * conv_taps[2]
    mixed = (out_gate.astype(F32) * conv_out).astype(BF)

    big = 2 * slots * depth * f
    pre_gate, pre_up = call(
        forward_kernel, ids, xs + [wg, wu], [sds((slots, f), F32)] * 2, 2 * big
    )
    hid_mine, hid_theirs = call(
        hidden_kernel, ids, [own_cot, wd, od], [sds((slots, f), F32)] * 2, big
    )
    hid_theirs = core_swap(hid_theirs)
    hact, gcat = call(
        grads_kernel,
        ids,
        [hid_mine, hid_theirs, pre_gate, pre_up],
        [sds((slots, f), BF), sds((slots, 2 * f), BF)],
        big // 10,
    )
    gother = core_swap(gcat)
    half = blk // 2
    part_list = call(
        partial_kernel,
        ids,
        [gcat, gother, wg, wu, og, ou],
        [sds((slots, half), BF)] * (2 * NZ),
        2 * big,
    )
    chunks = [dict(zip(STEPS, part_list[i::2])) for i in range(2)]
    for parts in chunks:
        parts[4] = parts[-4]

    mixed = jnp.roll(mixed, -c * (tok // 2), axis=0)
    mixed, _ = tied(mixed, own_cot)
    with jax.named_scope("mixed_send"):
        all_mixed = lax.all_to_all(
            jnp.broadcast_to(mixed[None], (experts, tok, blk)), "sp", 0, 0, tiled=True
        )

    slot_grad = jnp.concatenate(ring_scatter(chunks), axis=1).astype(BF)
    slot_grad, all_mixed = tied(slot_grad, all_mixed)
    returned = lax.all_to_all(
        slot_grad.reshape(experts, cap, blk), "sp", 0, 0, tiled=True
    ).reshape(slots, blk)
    gcat_late, slot_grad = tied(gcat, slot_grad)
    other_cot = core_swap(own_cot)
    hact, other_cot = tied(hact, other_cot)
    gg, gu, gd = call(
        weight_kernel,
        ids,
        xs + [own_cot, other_cot, gcat_late, hact],
        [sds((depth, f), F32), sds((depth, f), F32), sds((f, depth), F32)],
        3 * big,
    )
    returned, gg = tied(returned, gg)
    moe_grad = dot(select, returned, 0, 0)
    mixer_cot = (cotangent.astype(F32) + moe_grad).astype(BF)

    m_swapped = {}

    def swap_blocks(k, blocks):
        keys = (0,) if k == 1 else (1 - k, k - 1)
        m_swapped.update({j: core_swap(blocks[j]) for j in keys})
        return {j: m_swapped[j] for j in keys}

    m_own = ring_gather(mixer_cot, swap_blocks)
    m_swapped[-4] = core_swap(m_own[-4])
    ms = [m_own[j] for j in STEPS] + [m_swapped[j] for j in STEPS]
    (cols,) = call(columns_kernel, ids, ms, [sds((experts, tok // 2, blk), BF)], big // 10)
    with jax.named_scope("cols_send"):
        own_cols = lax.all_to_all(cols, "sp", 0, 0, tiled=True)
    out_proj, _ = tied(out_proj, cols)
    gog, gco = call(
        mixed_kernel,
        ids,
        ms + [out_proj, conv_out, out_gate],
        [sds((tok, blk), BF), sds((tok, blk), F32)],
        2 * tok * depth * blk,
    )

    prev, nxt = shifted(gco, *neighbours(gco[:1], gco[-1:]))
    gci = nxt * conv_taps[0] + gco * conv_taps[1] + prev * conv_taps[2]
    grad_in_gate = (gci * values.astype(F32)).astype(BF)
    grad_values = (gci * in_gate.astype(F32)).astype(BF)

    own_cols, gco = tied(own_cols, gco)
    other_cols = core_swap(own_cols)
    (grad_out_proj,) = call(
        proj_kernel,
        ids,
        [own_cols, other_cols, all_mixed],
        [sds((blk, blk), F32)],
        2 * tok * depth * blk,
    )
    return gog, grad_in_gate, grad_values, grad_out_proj, gg[None], gu[None], gd[None]


def solution(mesh):
    finer = Mesh(mesh.devices.reshape(mesh.shape["sp"], NZ, 2), ("sp", "z", "c"))
    rows = P("sp", ZC)
    cols = P(None, ZC)
    in_specs = (
        rows,
        rows,
        rows,
        rows,
        cols,
        cols,
        P("sp", None),
        P("sp", None),
        P("sp", None, ZC),
        P("sp", None, ZC),
        P("sp", ZC, None),
        rows,
    )
    out_specs = (rows, rows, rows, rows, P("sp", None, ZC), P("sp", None, ZC), P("sp", ZC, None))
    return jax.shard_map(body, mesh=finer, in_specs=in_specs, out_specs=out_specs, check_vma=False)
```

```python
import functools

import jax
import jax.numpy as jnp
from jax import lax
from jax.experimental import pallas as pl
from jax.experimental.pallas import tpu as pltpu
from jax.sharding import Mesh
from jax.sharding import PartitionSpec as P


BF = jnp.bfloat16
F32 = jnp.float32
NZ = 8
ZC = ("z", "c")
STEPS = (0, -1, -2, -3, -4, 1, 2, 3)
CORE_SWAP = [(0, 1), (1, 0)]


def tied(*arrays):
    return lax.optimization_barrier(arrays)


def along(sign):
    return [(z * 2 + c, (z + sign * (1 - 2 * c)) % NZ * 2 + c) for z in range(NZ) for c in range(2)]


def ring_gather(block, note=lambda k, blocks: None):
    blocks = {0: block}
    for k in range(1, 5):
        blocks[-k] = lax.ppermute(blocks[1 - k], ZC, along(1))
        if k < 4:
            blocks[k] = lax.ppermute(blocks[k - 1], ZC, along(-1))
            blocks[-k], blocks[k] = tied(blocks[-k], blocks[k])
        note(k, blocks)
    return blocks


def core_swap(array):
    return lax.ppermute(array, "c", CORE_SWAP)


def add_rounded(a, b):
    return (a.astype(F32) + b.astype(F32)).astype(BF)


def ring_scatter(parts):
    up, down = parts[4], parts[-3]
    for k in range(3, -1, -1):
        up = lax.ppermute(up, ZC, along(1))
        if k < 3:
            down = lax.ppermute(down, ZC, along(-1))
        if k:
            up = add_rounded(up, parts[k])
            if k < 3:
                down = add_rounded(down, parts[-k])
            up, down = tied(up, down)
    return parts[0].astype(F32) + up.astype(F32) + down.astype(F32)


def block_ids():
    z, c = lax.axis_index("z"), lax.axis_index("c")
    sgn = 1 - 2 * c
    own = [(z + sgn * j + NZ) % NZ * 2 + c for j in STEPS]
    other = [(z - sgn * j + NZ) % NZ * 2 + (1 - c) for j in STEPS]
    return jnp.stack(own + other).astype(jnp.int32)


def call(kernel, ids, args, outs, flops):
    vmem = pl.BlockSpec(memory_space=pltpu.VMEM)
    return pl.pallas_call(
        kernel,
        in_specs=[pl.BlockSpec(memory_space=pltpu.SMEM)] + [vmem] * len(args),
        out_specs=[vmem] * len(outs),
        out_shape=outs,
        cost_estimate=pl.CostEstimate(flops=flops, bytes_accessed=flops // 500, transcendentals=0),
    )(ids, *args)


def dot(a, b, ca, cb):
    return lax.dot_general(a, b, (((ca,), (cb,)), ((), ())), preferred_element_type=F32)


def rows_of(ids, i, width):
    return pl.ds(pl.multiple_of(ids[i] * width, width), width)


def forward_kernel(ids, *refs):
    xs, (wg, wu, og, ou, mine, theirs, x_all) = refs[:NZ], refs[NZ:]
    total = None
    for i, x in enumerate(xs):
        at = rows_of(ids, i, x.shape[1])
        w = jnp.concatenate([wg[at, :], wu[at, :], og[at, :], ou[at, :]], axis=1)
        x_all[i] = x[...]
        part = dot(x[...], w, 1, 0)
        total = part if total is None else total + part
    width = mine.shape[1]
    mine[...] = total[:, :width]
    theirs[...] = total[:, width:]


def hidden_kernel(ids, cot, wd, od, mine, theirs):
    f = wd.shape[0]
    width = cot.shape[1] // NZ
    mine[...] = jnp.zeros_like(mine)
    theirs[...] = jnp.zeros_like(theirs)

    def step(j, carry):
        here = pl.ds(pl.multiple_of(j * width, width), width)
        at = rows_of(ids, j, width)
        w = jnp.concatenate([wd[:, at], od[:, at]], axis=0)
        part = dot(cot[:, here], w, 1, 1)
        mine[...] += part[:, :f]
        theirs[...] += part[:, f:]
        return carry

    lax.fori_loop(0, NZ, step, 0)


def grads_kernel(ids, fmine, ftheirs, hmine, htheirs, hact, gcat):
    f = hmine.shape[1]
    total = hmine[...] + htheirs[...]
    gate = fmine[:, :f] + ftheirs[:, :f]
    up = fmine[:, f:] + ftheirs[:, f:]
    sig = jax.nn.sigmoid(gate)
    act = gate * sig
    hact[...] = (act * up).astype(BF)
    gcat[:, :f] = (total * up * sig * (1.0 + gate * (1.0 - sig))).astype(BF)
    gcat[:, f:] = (total * act).astype(BF)


def partial_kernel(ids, gcat, gother, wg, wu, og, ou, *parts):
    g = jnp.concatenate([gcat[...], gother[...]], axis=1)
    for i, part in enumerate(parts):
        at = rows_of(ids, i, part.shape[1])
        w = jnp.concatenate([wg[at, :], wu[at, :], og[at, :], ou[at, :]], axis=1)
        part[...] = dot(g, w, 1, 1).astype(BF)


def weight_kernel(ids, x_own, x_other, own, other, gcat, hact, gg, gu, gd):
    f = gg.shape[1]
    width = x_own.shape[2]

    def step(j, carry):
        for base, xs in ((0, x_own), (NZ, x_other)):
            both = dot(xs[j], gcat[...], 0, 0)
            at = rows_of(ids, base + j, width)
            gg[at, :] = both[:, :f]
            gu[at, :] = both[:, f:]
        here = pl.ds(pl.multiple_of(j * width, width), width)
        for base, cot in ((0, own), (NZ, other)):
            at = rows_of(ids, base + j, width)
            gd[:, at] = dot(hact[...], cot[:, here], 0, 0)
        return carry

    lax.fori_loop(0, NZ, step, 0)


def columns_kernel(ids, *refs):
    ms, cols = refs[:NZ], refs[NZ]
    width = cols.shape[2]
    for i, m in enumerate(ms):
        for p in range(2):
            cols[ids[i] // 2 * 2 + p] = m[:, p * width : (p + 1) * width]


def mixed_kernel(ids, *refs):
    ms, (proj, other_proj, mine, theirs) = refs[:NZ], refs[NZ:]
    total = None
    for i, m in enumerate(ms):
        wide = m.shape[1]
        at = pl.ds(pl.multiple_of(ids[i] // 2 * wide, wide), wide)
        w = jnp.concatenate([proj[at, :], other_proj[at, :]], axis=1)
        part = dot(m[...], w, 1, 0)
        total = part if total is None else total + part
    width = mine.shape[1]
    mine[...] = total[:, :width]
    theirs[...] = total[:, width:]


def proj_kernel(ids, own, other, mixed, out):
    groups, half, width = own.shape

    def part(cols, at):
        rows = mixed[:, at : at + half, :]
        flat = (groups * half, width)
        return dot(cols[...].reshape(flat), rows.reshape(flat), 0, 0)

    out[...] = part(own, 0) + part(other, half)


def neighbours(first, last):
    size = lax.axis_size("sp")
    up = [(i, i + 1) for i in range(size - 1)]
    return lax.ppermute(last, "sp", up), lax.ppermute(first, "sp", [(j, i) for i, j in up])


def shifted(array, before, after):
    return jnp.concatenate([before, array[:-1]], axis=0), jnp.concatenate([array[1:], after], axis=0)


def sds(shape, dtype):
    return jax.ShapeDtypeStruct(shape, dtype)


def body(
    moe_input,
    out_gate,
    in_gate,
    values,
    conv_taps,
    out_proj,
    route_ids,
    route_gates,
    expert_gate,
    expert_up,
    expert_down,
    cotangent,
):
    tok, blk = moe_input.shape
    experts = lax.axis_size("sp")
    cap = 3 * tok // experts
    slots = experts * cap
    c = lax.axis_index("c")
    ids = block_ids()
    wg, wu, wd = expert_gate[0], expert_up[0], expert_down[0]
    depth, f = wg.shape

    cot_blocks = ring_gather(cotangent)
    cot_tokens = jnp.concatenate([cot_blocks[j] for j in STEPS], axis=1)

    ids_t = route_ids.T
    gates_t = route_gates.T
    which = jnp.arange(experts, dtype=jnp.int32)[:, None]
    hit = [ids_t[k][None, :] == which for k in range(ids_t.shape[0])]
    chosen = functools.reduce(jnp.logical_or, hit)
    weight = sum(jnp.where(h, gates_t[k][None, :], 0.0) for k, h in enumerate(hit))
    t = jnp.arange(tok, dtype=jnp.int32)
    before = (t[:, None] < t[None, :]).astype(BF)
    position = jnp.dot(chosen.astype(BF), before, preferred_element_type=F32).astype(jnp.int32)
    place = jnp.where(chosen, position, -1)
    pick = place[:, None, :] == jnp.arange(cap, dtype=jnp.int32)[None, :, None]
    select = pick.astype(BF).reshape(slots, tok)
    slot_weight = jnp.sum(jnp.where(pick, weight[:, None, :], 0.0), axis=2).reshape(slots, 1)

    send_x = jnp.dot(select, moe_input, preferred_element_type=F32).astype(BF)
    x0 = lax.all_to_all(send_x.reshape(experts, cap, blk), "sp", 0, 0, tiled=True)
    x0 = x0.reshape(slots, blk)
    send_c = (
        slot_weight * jnp.dot(select, cot_tokens, preferred_element_type=F32)
    ).astype(BF)

    og, ou, od = (core_swap(w) for w in (wg, wu, wd))
    other_proj = core_swap(out_proj)
    conv_in = in_gate.astype(F32) * values.astype(F32)
    held = {}

    def note(k, blocks):
        if k == 1:
            blocks[-1], blocks[1], held["conv_in"] = tied(blocks[-1], blocks[1], conv_in)

    x_own = ring_gather(x0, note)
    send_c, x0 = tied(send_c, x0)
    own_cot = lax.all_to_all(
        send_c.reshape(experts, cap, NZ * blk), "sp", 0, 0, tiled=True
    ).reshape(slots, NZ * blk)
    conv_in = held["conv_in"]
    conv_ends = neighbours(conv_in[:1], conv_in[-1:])
    own_cot, *conv_ends = tied(own_cot, *conv_ends)
    prev, nxt = shifted(conv_in, *conv_ends)
    conv_out = prev * conv_taps[0] + conv_in * conv_taps[1] + nxt * conv_taps[2]
    mixed = (out_gate.astype(F32) * conv_out).astype(BF)
    rolled = jnp.roll(mixed, -c * (tok // 2), axis=0)
    all_mixed = lax.all_to_all(
        jnp.broadcast_to(rolled[None], (experts, tok, blk)), "sp", 0, 0, tiled=True
    )

    big = 2 * slots * depth * f
    fwd_mine, fwd_theirs, x_all = call(
        forward_kernel,
        ids,
        [x_own[j] for j in STEPS] + [wg, wu, og, ou],
        [sds((slots, 2 * f), F32)] * 2 + [sds((NZ, slots, blk), BF)],
        2 * big,
    )
    fwd_theirs = core_swap(fwd_theirs)
    x_other = core_swap(x_all)
    own_cot, x_other = tied(own_cot, x_other)
    hid_mine, hid_theirs = call(
        hidden_kernel, ids, [own_cot, wd, od], [sds((slots, f), F32)] * 2, big
    )
    hid_theirs = core_swap(hid_theirs)
    hact, gcat = call(
        grads_kernel,
        ids,
        [fwd_mine, fwd_theirs, hid_mine, hid_theirs],
        [sds((slots, f), BF), sds((slots, 2 * f), BF)],
        big // 10,
    )
    gother = core_swap(gcat)
    part_list = call(
        partial_kernel,
        ids,
        [gcat, gother, wg, wu, og, ou],
        [sds((slots, blk), BF)] * NZ,
        2 * big,
    )
    parts = dict(zip(STEPS, part_list))
    parts[4] = parts[-4]

    slot_grad = ring_scatter(parts).astype(BF)
    slot_grad, all_mixed = tied(slot_grad, all_mixed)
    returned = lax.all_to_all(
        slot_grad.reshape(experts, cap, blk), "sp", 0, 0, tiled=True
    ).reshape(slots, blk)
    own_cot_late, slot_grad = tied(own_cot, slot_grad)
    other_cot = core_swap(own_cot_late)
    gg, gu, gd = call(
        weight_kernel,
        ids,
        [x_all, x_other, own_cot, other_cot, gcat, hact],
        [sds((depth, f), F32), sds((depth, f), F32), sds((f, depth), F32)],
        3 * big,
    )
    returned, gg = tied(returned, gg)
    moe_grad = dot(select, returned, 0, 0)
    mixer_cot = (cotangent.astype(F32) + moe_grad).astype(BF)

    half = tok // 2
    here = lax.dynamic_slice_in_dim(mixer_cot, c * half, half, 0)
    there = lax.dynamic_slice_in_dim(mixer_cot, (1 - c) * half, half, 0)
    got = core_swap(there)
    pair = jnp.where(
        c == 0, jnp.concatenate([here, got], axis=1), jnp.concatenate([got, here], axis=1)
    )
    m_own = ring_gather(pair)
    ms = [m_own[j] for j in STEPS]
    (cols,) = call(columns_kernel, ids, ms, [sds((experts, half, blk), BF)], big // 100)
    out_proj, _ = tied(out_proj, cols)
    mixed_mine, mixed_theirs = call(
        mixed_kernel,
        ids,
        ms + [out_proj, other_proj],
        [sds((half, blk), F32)] * 2,
        2 * tok * depth * blk,
    )
    own_cols = lax.all_to_all(cols, "sp", 0, 0, tiled=True)
    mixed_got = core_swap(mixed_theirs)
    grad_mixed = jnp.where(
        c == 0,
        jnp.concatenate([mixed_mine, mixed_got], axis=0),
        jnp.concatenate([mixed_got, mixed_mine], axis=0),
    )
    gog = (grad_mixed * conv_out).astype(BF)
    gco = grad_mixed * out_gate.astype(F32)

    ends = neighbours(gco[:1], gco[-1:])
    own_cols, *ends = tied(own_cols, *ends)
    prev, nxt = shifted(gco, *ends)
    gci = nxt * conv_taps[0] + gco * conv_taps[1] + prev * conv_taps[2]
    grad_in_gate = (gci * values.astype(F32)).astype(BF)
    grad_values = (gci * in_gate.astype(F32)).astype(BF)

    other_cols = core_swap(own_cols)
    (grad_out_proj,) = call(
        proj_kernel,
        ids,
        [own_cols, other_cols, all_mixed],
        [sds((blk, blk), F32)],
        2 * tok * depth * blk,
    )
    return gog, grad_in_gate, grad_values, grad_out_proj, gg[None], gu[None], gd[None]


def solution(mesh):
    finer = Mesh(mesh.devices.reshape(mesh.shape["sp"], NZ, 2), ("sp", "z", "c"))
    rows = P("sp", ZC)
    cols = P(None, ZC)
    in_specs = (
        rows,
        rows,
        rows,
        rows,
        cols,
        cols,
        P("sp", None),
        P("sp", None),
        P("sp", None, ZC),
        P("sp", None, ZC),
        P("sp", ZC, None),
        rows,
    )
    out_specs = (rows, rows, rows, rows, P("sp", None, ZC), P("sp", None, ZC), P("sp", ZC, None))
    return jax.shard_map(body, mesh=finer, in_specs=in_specs, out_specs=out_specs, check_vma=False)
```

```python
import functools

import jax
import jax.numpy as jnp
from jax import lax
from jax.experimental import pallas as pl
from jax.experimental.pallas import tpu as pltpu
from jax.sharding import Mesh
from jax.sharding import PartitionSpec as P


BF = jnp.bfloat16
F32 = jnp.float32
NZ = 8
ZC = ("z", "c")
STEPS = (0, -1, -2, -3, -4, 1, 2, 3)
CORE_SWAP = [(0, 1), (1, 0)]


def tied(*arrays):
    return lax.optimization_barrier(arrays)


def along(sign):
    return [(z * 2 + c, (z + sign * (1 - 2 * c)) % NZ * 2 + c) for z in range(NZ) for c in range(2)]


def ring_gather(block, note=lambda k, blocks: None):
    blocks = {0: block}
    for k in range(1, 5):
        blocks[-k] = lax.ppermute(blocks[1 - k], ZC, along(1))
        if k < 4:
            blocks[k] = lax.ppermute(blocks[k - 1], ZC, along(-1))
            blocks[-k], blocks[k] = tied(blocks[-k], blocks[k])
        note(k, blocks)
    return blocks


def core_swap(array):
    return lax.ppermute(array, "c", CORE_SWAP)


def add_rounded(a, b):
    return (a.astype(F32) + b.astype(F32)).astype(BF)


def ring_scatter(parts):
    up, down = parts[4], parts[-3]
    for k in range(3, -1, -1):
        up = lax.ppermute(up, ZC, along(1))
        if k < 3:
            down = lax.ppermute(down, ZC, along(-1))
        if k:
            up = add_rounded(up, parts[k])
            if k < 3:
                down = add_rounded(down, parts[-k])
            up, down = tied(up, down)
    return parts[0].astype(F32) + up.astype(F32) + down.astype(F32)


def block_ids():
    z, c = lax.axis_index("z"), lax.axis_index("c")
    sgn = 1 - 2 * c
    own = [(z + sgn * j + NZ) % NZ * 2 + c for j in STEPS]
    other = [(z - sgn * j + NZ) % NZ * 2 + (1 - c) for j in STEPS]
    return jnp.stack(own + other).astype(jnp.int32)


def room(args, outs):
    return sum(a.size * a.dtype.itemsize for a in (*args, *outs)) * 3 // 2 + (4 << 20)


def call(kernel, ids, args, outs, flops, tight=False):
    vmem = pl.BlockSpec(memory_space=pltpu.VMEM)
    return pl.pallas_call(
        kernel,
        in_specs=[pl.BlockSpec(memory_space=pltpu.SMEM)] + [vmem] * len(args),
        out_specs=[vmem] * len(outs),
        out_shape=outs,
        cost_estimate=pl.CostEstimate(flops=flops, bytes_accessed=flops // 500, transcendentals=0),
        compiler_params=pltpu.CompilerParams(vmem_limit_bytes=room(args, outs) if tight else None),
    )(ids, *args)


def dot(a, b, ca, cb):
    return lax.dot_general(a, b, (((ca,), (cb,)), ((), ())), preferred_element_type=F32)


def rows_of(ids, i, width):
    return pl.ds(pl.multiple_of(ids[i] * width, width), width)


def forward_kernel(ids, *refs):
    xs, (wg, wu, og, ou, mine, theirs, x_all) = refs[:NZ], refs[NZ:]
    total = None
    for i, x in enumerate(xs):
        at = rows_of(ids, i, x.shape[1])
        w = jnp.concatenate([wg[at, :], wu[at, :], og[at, :], ou[at, :]], axis=1)
        x_all[i] = x[...]
        part = dot(x[...], w, 1, 0)
        total = part if total is None else total + part
    width = mine.shape[1]
    mine[...] = total[:, :width]
    theirs[...] = total[:, width:]


def hidden_kernel(ids, cot, wd, od, fwd_theirs, mine, theirs):
    f = wd.shape[0]
    width = cot.shape[1] // NZ
    mine[...] = jnp.zeros_like(mine)
    theirs[:, : 2 * f] = fwd_theirs[...]
    theirs[:, 2 * f :] = jnp.zeros_like(mine)

    def step(j, carry):
        here = pl.ds(pl.multiple_of(j * width, width), width)
        at = rows_of(ids, j, width)
        w = jnp.concatenate([wd[:, at], od[:, at]], axis=0)
        part = dot(cot[:, here], w, 1, 1)
        mine[...] += part[:, :f]
        theirs[:, 2 * f :] += part[:, f:]
        return carry

    lax.fori_loop(0, NZ, step, 0)


def grads_kernel(ids, fmine, hmine, theirs, hact, gcat):
    f = hmine.shape[1]
    total = hmine[...] + theirs[:, 2 * f :]
    gate = fmine[:, :f] + theirs[:, :f]
    up = fmine[:, f:] + theirs[:, f : 2 * f]
    sig = jax.nn.sigmoid(gate)
    act = gate * sig
    hact[...] = (act * up).astype(BF)
    gcat[:, :f] = (total * up * sig * (1.0 + gate * (1.0 - sig))).astype(BF)
    gcat[:, f:] = (total * act).astype(BF)


def partial_kernel(ids, gcat, gother, wg, wu, og, ou, *parts):
    g = jnp.concatenate([gcat[...], gother[...]], axis=1)
    for i, part in enumerate(parts):
        at = rows_of(ids, i, part.shape[1])
        w = jnp.concatenate([wg[at, :], wu[at, :], og[at, :], ou[at, :]], axis=1)
        part[...] = dot(g, w, 1, 1).astype(BF)


def weight_kernel(ids, x_own, x_other, own, other, gcat, hact, gg, gu, gd):
    f = gg.shape[1]
    width = x_own.shape[2]

    def step(j, carry):
        for base, xs in ((0, x_own), (NZ, x_other)):
            both = dot(xs[j], gcat[...], 0, 0)
            at = rows_of(ids, base + j, width)
            gg[at, :] = both[:, :f]
            gu[at, :] = both[:, f:]
        here = pl.ds(pl.multiple_of(j * width, width), width)
        for base, cot in ((0, own), (NZ, other)):
            at = rows_of(ids, base + j, width)
            gd[:, at] = dot(hact[...], cot[:, here], 0, 0)
        return carry

    lax.fori_loop(0, NZ, step, 0)


def columns_kernel(ids, *refs):
    ms, cols = refs[:NZ], refs[NZ]
    width = cols.shape[2]
    for i, m in enumerate(ms):
        for p in range(2):
            cols[ids[i] // 2 * 2 + p] = m[:, p * width : (p + 1) * width]


def mixed_kernel(ids, *refs):
    ms, (proj, other_proj, mine, theirs) = refs[:NZ], refs[NZ:]
    total = None
    for i, m in enumerate(ms):
        wide = m.shape[1]
        at = pl.ds(pl.multiple_of(ids[i] // 2 * wide, wide), wide)
        w = jnp.concatenate([proj[at, :], other_proj[at, :]], axis=1)
        part = dot(m[...], w, 1, 0)
        total = part if total is None else total + part
    width = mine.shape[1]
    mine[...] = total[:, :width]
    theirs[...] = total[:, width:]


def proj_kernel(ids, own, other, mixed, out):
    groups, half, width = own.shape

    def part(cols, at):
        rows = mixed[:, at : at + half, :]
        flat = (groups * half, width)
        return dot(cols[...].reshape(flat), rows.reshape(flat), 0, 0)

    out[...] = part(own, 0) + part(other, half)


def neighbours(first, last):
    size = lax.axis_size("sp")
    up = [(i, i + 1) for i in range(size - 1)]
    return lax.ppermute(last, "sp", up), lax.ppermute(first, "sp", [(j, i) for i, j in up])


def shifted(array, before, after):
    return jnp.concatenate([before, array[:-1]], axis=0), jnp.concatenate([array[1:], after], axis=0)


def sds(shape, dtype):
    return jax.ShapeDtypeStruct(shape, dtype)


def body(
    moe_input,
    out_gate,
    in_gate,
    values,
    conv_taps,
    out_proj,
    route_ids,
    route_gates,
    expert_gate,
    expert_up,
    expert_down,
    cotangent,
):
    tok, blk = moe_input.shape
    experts = lax.axis_size("sp")
    cap = 3 * tok // experts
    slots = experts * cap
    c = lax.axis_index("c")
    ids = block_ids()
    wg, wu, wd = expert_gate[0], expert_up[0], expert_down[0]
    depth, f = wg.shape

    cot_blocks = ring_gather(cotangent)
    cot_tokens = jnp.concatenate([cot_blocks[j] for j in STEPS], axis=1)

    ids_t = route_ids.T
    gates_t = route_gates.T
    which = jnp.arange(experts, dtype=jnp.int32)[:, None]
    hit = [ids_t[k][None, :] == which for k in range(ids_t.shape[0])]
    chosen = functools.reduce(jnp.logical_or, hit)
    weight = sum(jnp.where(h, gates_t[k][None, :], 0.0) for k, h in enumerate(hit))
    t = jnp.arange(tok, dtype=jnp.int32)
    before = (t[:, None] < t[None, :]).astype(BF)
    position = jnp.dot(chosen.astype(BF), before, preferred_element_type=F32).astype(jnp.int32)
    place = jnp.where(chosen, position, -1)
    pick = place[:, None, :] == jnp.arange(cap, dtype=jnp.int32)[None, :, None]
    select = pick.astype(BF).reshape(slots, tok)
    slot_weight = jnp.sum(jnp.where(pick, weight[:, None, :], 0.0), axis=2).reshape(slots, 1)

    send_x = jnp.dot(select, moe_input, preferred_element_type=F32).astype(BF)
    x0 = lax.all_to_all(send_x.reshape(experts, cap, blk), "sp", 0, 0, tiled=True)
    x0 = x0.reshape(slots, blk)
    send_c = (
        slot_weight * jnp.dot(select, cot_tokens, preferred_element_type=F32)
    ).astype(BF)

    og, ou, od = (core_swap(w) for w in (wg, wu, wd))
    other_proj = core_swap(out_proj)
    conv_in = in_gate.astype(F32) * values.astype(F32)
    held = {}

    def note(k, blocks):
        if k == 1:
            blocks[-1], blocks[1], held["conv_in"] = tied(blocks[-1], blocks[1], conv_in)

    x_own = ring_gather(x0, note)
    send_c, x0 = tied(send_c, x0)
    own_cot = lax.all_to_all(
        send_c.reshape(experts, cap, NZ * blk), "sp", 0, 0, tiled=True
    ).reshape(slots, NZ * blk)
    conv_in = held["conv_in"]
    conv_ends = neighbours(conv_in[:1], conv_in[-1:])
    own_cot, *conv_ends = tied(own_cot, *conv_ends)
    prev, nxt = shifted(conv_in, *conv_ends)
    conv_out = prev * conv_taps[0] + conv_in * conv_taps[1] + nxt * conv_taps[2]
    mixed = (out_gate.astype(F32) * conv_out).astype(BF)
    rolled = jnp.roll(mixed, -c * (tok // 2), axis=0)
    all_mixed = lax.all_to_all(
        jnp.broadcast_to(rolled[None], (experts, tok, blk)), "sp", 0, 0, tiled=True
    )

    big = 2 * slots * depth * f
    fwd_mine, fwd_theirs, x_all = call(
        forward_kernel,
        ids,
        [x_own[j] for j in STEPS] + [wg, wu, og, ou],
        [sds((slots, 2 * f), F32)] * 2 + [sds((NZ, slots, blk), BF)],
        2 * big,
    )
    x_other = core_swap(x_all)
    own_cot, x_other = tied(own_cot, x_other)
    hid_mine, theirs = call(
        hidden_kernel,
        ids,
        [own_cot, wd, od, fwd_theirs],
        [sds((slots, f), F32), sds((slots, 3 * f), F32)],
        big,
        tight=True,
    )
    theirs = core_swap(theirs)
    hact, gcat = call(
        grads_kernel,
        ids,
        [fwd_mine, hid_mine, theirs],
        [sds((slots, f), BF), sds((slots, 2 * f), BF)],
        big // 10,
        tight=True,
    )
    gother = core_swap(gcat)
    part_list = call(
        partial_kernel,
        ids,
        [gcat, gother, wg, wu, og, ou],
        [sds((slots, blk), BF)] * NZ,
        2 * big,
    )
    parts = dict(zip(STEPS, part_list))
    parts[4] = parts[-4]

    slot_grad = ring_scatter(parts).astype(BF)
    slot_grad, all_mixed = tied(slot_grad, all_mixed)
    returned = lax.all_to_all(
        slot_grad.reshape(experts, cap, blk), "sp", 0, 0, tiled=True
    ).reshape(slots, blk)
    own_cot_late, slot_grad = tied(own_cot, slot_grad)
    other_cot = core_swap(own_cot_late)
    gg, gu, gd = call(
        weight_kernel,
        ids,
        [x_all, x_other, own_cot, other_cot, gcat, hact],
        [sds((depth, f), F32), sds((depth, f), F32), sds((f, depth), F32)],
        3 * big,
    )
    returned, gg = tied(returned, gg)
    moe_grad = dot(select, returned, 0, 0)
    mixer_cot = (cotangent.astype(F32) + moe_grad).astype(BF)

    half = tok // 2
    here = lax.dynamic_slice_in_dim(mixer_cot, c * half, half, 0)
    there = lax.dynamic_slice_in_dim(mixer_cot, (1 - c) * half, half, 0)
    got = core_swap(there)
    pair = jnp.where(
        c == 0, jnp.concatenate([here, got], axis=1), jnp.concatenate([got, here], axis=1)
    )
    m_own = ring_gather(pair)
    ms = [m_own[j] for j in STEPS]
    (cols,) = call(columns_kernel, ids, ms, [sds((experts, half, blk), BF)], big // 100, tight=True)
    out_proj, _ = tied(out_proj, cols)
    mixed_mine, mixed_theirs = call(
        mixed_kernel,
        ids,
        ms + [out_proj, other_proj],
        [sds((half, blk), F32)] * 2,
        2 * tok * depth * blk,
    )
    own_cols = lax.all_to_all(cols, "sp", 0, 0, tiled=True)
    mixed_got = core_swap(mixed_theirs)
    grad_mixed = jnp.where(
        c == 0,
        jnp.concatenate([mixed_mine, mixed_got], axis=0),
        jnp.concatenate([mixed_got, mixed_mine], axis=0),
    )
    gog = (grad_mixed * conv_out).astype(BF)
    gco = grad_mixed * out_gate.astype(F32)

    ends = neighbours(gco[:1], gco[-1:])
    own_cols, *ends = tied(own_cols, *ends)
    prev, nxt = shifted(gco, *ends)
    gci = nxt * conv_taps[0] + gco * conv_taps[1] + prev * conv_taps[2]
    grad_in_gate = (gci * values.astype(F32)).astype(BF)
    grad_values = (gci * in_gate.astype(F32)).astype(BF)

    other_cols = core_swap(own_cols)
    (grad_out_proj,) = call(
        proj_kernel,
        ids,
        [own_cols, other_cols, all_mixed],
        [sds((blk, blk), F32)],
        2 * tok * depth * blk,
        tight=True,
    )
    return gog, grad_in_gate, grad_values, grad_out_proj, gg[None], gu[None], gd[None]


def solution(mesh):
    finer = Mesh(mesh.devices.reshape(mesh.shape["sp"], NZ, 2), ("sp", "z", "c"))
    rows = P("sp", ZC)
    cols = P(None, ZC)
    in_specs = (
        rows,
        rows,
        rows,
        rows,
        cols,
        cols,
        P("sp", None),
        P("sp", None),
        P("sp", None, ZC),
        P("sp", None, ZC),
        P("sp", ZC, None),
        rows,
    )
    out_specs = (rows, rows, rows, rows, P("sp", None, ZC), P("sp", None, ZC), P("sp", ZC, None))
    return jax.shard_map(body, mesh=finer, in_specs=in_specs, out_specs=out_specs, check_vma=False)
```

```python
import functools

import jax
import jax.numpy as jnp
from jax import lax
from jax.experimental import pallas as pl
from jax.experimental.pallas import tpu as pltpu
from jax.sharding import Mesh
from jax.sharding import PartitionSpec as P


BF = jnp.bfloat16
F32 = jnp.float32
NZ = 8
ZC = ("z", "c")
STEPS = (0, -1, -2, -3, -4, 1, 2, 3)
CORE_SWAP = [(0, 1), (1, 0)]


def tied(*arrays):
    return lax.optimization_barrier(arrays)


def along(sign):
    return [(z * 2 + c, (z + sign * (1 - 2 * c)) % NZ * 2 + c) for z in range(NZ) for c in range(2)]


def ring_gather(block, note=lambda k, blocks: None):
    blocks = {0: block}
    for k in range(1, 5):
        blocks[-k] = lax.ppermute(blocks[1 - k], ZC, along(1))
        if k < 4:
            blocks[k] = lax.ppermute(blocks[k - 1], ZC, along(-1))
            blocks[-k], blocks[k] = tied(blocks[-k], blocks[k])
        note(k, blocks)
    return blocks


def core_swap(array):
    return lax.ppermute(array, "c", CORE_SWAP)


def add_rounded(a, b):
    return (a.astype(F32) + b.astype(F32)).astype(BF)


def ring_scatter(parts):
    up, down = parts[4], parts[-3]
    for k in range(3, -1, -1):
        up = lax.ppermute(up, ZC, along(1))
        if k < 3:
            down = lax.ppermute(down, ZC, along(-1))
        if k:
            up = add_rounded(up, parts[k])
            if k < 3:
                down = add_rounded(down, parts[-k])
            up, down = tied(up, down)
    return parts[0].astype(F32) + up.astype(F32) + down.astype(F32)


def block_ids():
    z, c = lax.axis_index("z"), lax.axis_index("c")
    sgn = 1 - 2 * c
    own = [(z + sgn * j + NZ) % NZ * 2 + c for j in STEPS]
    other = [(z - sgn * j + NZ) % NZ * 2 + (1 - c) for j in STEPS]
    return jnp.stack(own + other).astype(jnp.int32)


def room(args, outs):
    return sum(a.size * a.dtype.itemsize for a in (*args, *outs)) * 3 // 2 + (4 << 20)


def call(kernel, ids, args, outs, flops, tight=False):
    vmem = pl.BlockSpec(memory_space=pltpu.VMEM)
    return pl.pallas_call(
        kernel,
        in_specs=[pl.BlockSpec(memory_space=pltpu.SMEM)] + [vmem] * len(args),
        out_specs=[vmem] * len(outs),
        out_shape=outs,
        cost_estimate=pl.CostEstimate(flops=flops, bytes_accessed=flops // 500, transcendentals=0),
        compiler_params=pltpu.CompilerParams(vmem_limit_bytes=room(args, outs) if tight else None),
    )(ids, *args)


def dot(a, b, ca, cb):
    return lax.dot_general(a, b, (((ca,), (cb,)), ((), ())), preferred_element_type=F32)


def rows_of(ids, i, width):
    return pl.ds(pl.multiple_of(ids[i] * width, width), width)


def forward_kernel(ids, *refs):
    xs, (wg, wu, og, ou, mine, theirs, x_all) = refs[:NZ], refs[NZ:]
    total = None
    for i, x in enumerate(xs):
        at = rows_of(ids, i, x.shape[1])
        w = jnp.concatenate([wg[at, :], wu[at, :], og[at, :], ou[at, :]], axis=1)
        x_all[i] = x[...]
        part = dot(x[...], w, 1, 0)
        total = part if total is None else total + part
    width = mine.shape[1]
    mine[...] = total[:, :width]
    theirs[...] = total[:, width:]


def hidden_kernel(ids, cot, wd, od, fwd_theirs, mine, theirs):
    f = wd.shape[0]
    width = cot.shape[1] // NZ
    mine[...] = jnp.zeros_like(mine)
    theirs[:, : 2 * f] = fwd_theirs[...]
    theirs[:, 2 * f :] = jnp.zeros_like(mine)

    def step(j, carry):
        here = pl.ds(pl.multiple_of(j * width, width), width)
        at = rows_of(ids, j, width)
        w = jnp.concatenate([wd[:, at], od[:, at]], axis=0)
        part = dot(cot[:, here], w, 1, 1)
        mine[...] += part[:, :f]
        theirs[:, 2 * f :] += part[:, f:]
        return carry

    lax.fori_loop(0, NZ, step, 0)


def grads_kernel(ids, fmine, hmine, theirs, hact, gcat):
    f = hmine.shape[1]
    total = hmine[...] + theirs[:, 2 * f :]
    gate = fmine[:, :f] + theirs[:, :f]
    up = fmine[:, f:] + theirs[:, f : 2 * f]
    sig = jax.nn.sigmoid(gate)
    act = gate * sig
    hact[...] = (act * up).astype(BF)
    gcat[:, :f] = (total * up * sig * (1.0 + gate * (1.0 - sig))).astype(BF)
    gcat[:, f:] = (total * act).astype(BF)


def partial_kernel(ids, gcat, gother, wg, wu, og, ou, *parts):
    g = jnp.concatenate([gcat[...], gother[...]], axis=1)
    for i, part in enumerate(parts):
        at = rows_of(ids, i, part.shape[1])
        w = jnp.concatenate([wg[at, :], wu[at, :], og[at, :], ou[at, :]], axis=1)
        part[...] = dot(g, w, 1, 1).astype(BF)


def weight_kernel(ids, x_own, x_other, own, other, gcat, hact, gg, gu, gd):
    f = gg.shape[1]
    width = x_own.shape[2]

    def step(j, carry):
        for base, xs in ((0, x_own), (NZ, x_other)):
            both = dot(xs[j], gcat[...], 0, 0)
            at = rows_of(ids, base + j, width)
            gg[at, :] = both[:, :f]
            gu[at, :] = both[:, f:]
        here = pl.ds(pl.multiple_of(j * width, width), width)
        for base, cot in ((0, own), (NZ, other)):
            at = rows_of(ids, base + j, width)
            gd[:, at] = dot(hact[...], cot[:, here], 0, 0)
        return carry

    lax.fori_loop(0, NZ, step, 0)


def columns_kernel(ids, *refs):
    ms, cols = refs[:NZ], refs[NZ]
    width = cols.shape[2]
    for i, m in enumerate(ms):
        for p in range(2):
            cols[ids[i] // 2 * 2 + p] = m[:, p * width : (p + 1) * width]


def mixed_kernel(ids, *refs):
    ms, (proj, other_proj, mine, theirs) = refs[:NZ], refs[NZ:]
    total = None
    for i, m in enumerate(ms):
        wide = m.shape[1]
        at = pl.ds(pl.multiple_of(ids[i] // 2 * wide, wide), wide)
        w = jnp.concatenate([proj[at, :], other_proj[at, :]], axis=1)
        part = dot(m[...], w, 1, 0)
        total = part if total is None else total + part
    width = mine.shape[1]
    mine[...] = total[:, :width]
    theirs[...] = total[:, width:]


def proj_kernel(ids, own, other, mixed, out):
    groups, half, width = own.shape

    def part(cols, at):
        rows = mixed[:, at : at + half, :]
        flat = (groups * half, width)
        return dot(cols[...].reshape(flat), rows.reshape(flat), 0, 0)

    out[...] = part(own, 0) + part(other, half)


def neighbours(first, last):
    size = lax.axis_size("sp")
    up = [(i, i + 1) for i in range(size - 1)]
    return lax.ppermute(last, "sp", up), lax.ppermute(first, "sp", [(j, i) for i, j in up])


def shifted(array, before, after):
    return jnp.concatenate([before, array[:-1]], axis=0), jnp.concatenate([array[1:], after], axis=0)


def sds(shape, dtype):
    return jax.ShapeDtypeStruct(shape, dtype)


def body(
    moe_input,
    out_gate,
    in_gate,
    values,
    conv_taps,
    out_proj,
    route_ids,
    route_gates,
    expert_gate,
    expert_up,
    expert_down,
    cotangent,
):
    tok, blk = moe_input.shape
    experts = lax.axis_size("sp")
    cap = 3 * tok // experts
    slots = experts * cap
    c = lax.axis_index("c")
    ids = block_ids()
    wg, wu, wd = expert_gate[0], expert_up[0], expert_down[0]
    depth, f = wg.shape

    cot_blocks = ring_gather(cotangent)
    cot_tokens = jnp.concatenate([cot_blocks[j] for j in STEPS], axis=1)

    ids_t = route_ids.T
    gates_t = route_gates.T
    which = jnp.arange(experts, dtype=jnp.int32)[:, None]
    hit = [ids_t[k][None, :] == which for k in range(ids_t.shape[0])]
    chosen = functools.reduce(jnp.logical_or, hit)
    weight = sum(jnp.where(h, gates_t[k][None, :], 0.0) for k, h in enumerate(hit))
    t = jnp.arange(tok, dtype=jnp.int32)
    before = (t[:, None] < t[None, :]).astype(BF)
    position = jnp.dot(chosen.astype(BF), before, preferred_element_type=F32).astype(jnp.int32)
    place = jnp.where(chosen, position, -1)
    pick = place[:, None, :] == jnp.arange(cap, dtype=jnp.int32)[None, :, None]
    select = pick.astype(BF).reshape(slots, tok)
    slot_weight = jnp.sum(jnp.where(pick, weight[:, None, :], 0.0), axis=2).reshape(slots, 1)

    send_x = jnp.dot(select, moe_input, preferred_element_type=F32).astype(BF)
    x0 = lax.all_to_all(send_x.reshape(experts, cap, blk), "sp", 0, 0, tiled=True)
    x0 = x0.reshape(slots, blk)
    send_c = (
        slot_weight * jnp.dot(select, cot_tokens, preferred_element_type=F32)
    ).astype(BF)

    og, ou, od = (core_swap(w) for w in (wg, wu, wd))
    other_proj = core_swap(out_proj)
    conv_in = in_gate.astype(F32) * values.astype(F32)
    held = {}

    def note(k, blocks):
        if k == 1:
            blocks[-1], blocks[1], held["conv_in"], held["od"] = tied(
                blocks[-1], blocks[1], conv_in, od
            )

    x_own = ring_gather(x0, note)
    send_c, x0 = tied(send_c, x0)
    own_cot = lax.all_to_all(
        send_c.reshape(experts, cap, NZ * blk), "sp", 0, 0, tiled=True
    ).reshape(slots, NZ * blk)
    conv_in, od = held["conv_in"], held["od"]
    conv_ends = neighbours(conv_in[:1], conv_in[-1:])
    own_cot, *conv_ends = tied(own_cot, *conv_ends)
    prev, nxt = shifted(conv_in, *conv_ends)
    conv_out = prev * conv_taps[0] + conv_in * conv_taps[1] + nxt * conv_taps[2]
    mixed = (out_gate.astype(F32) * conv_out).astype(BF)
    rolled = jnp.roll(mixed, -c * (tok // 2), axis=0)
    all_mixed = lax.all_to_all(
        jnp.broadcast_to(rolled[None], (experts, tok, blk)), "sp", 0, 0, tiled=True
    )

    big = 2 * slots * depth * f
    fwd_mine, fwd_theirs, x_all = call(
        forward_kernel,
        ids,
        [x_own[j] for j in STEPS] + [wg, wu, og, ou],
        [sds((slots, 2 * f), F32)] * 2 + [sds((NZ, slots, blk), BF)],
        2 * big,
    )
    x_other = core_swap(x_all)
    hid_mine, theirs = call(
        hidden_kernel,
        ids,
        [own_cot, wd, od, fwd_theirs],
        [sds((slots, f), F32), sds((slots, 3 * f), F32)],
        big,
        tight=True,
    )
    theirs = core_swap(theirs)
    theirs, x_other = tied(theirs, x_other)
    hact, gcat = call(
        grads_kernel,
        ids,
        [fwd_mine, hid_mine, theirs],
        [sds((slots, f), BF), sds((slots, 2 * f), BF)],
        big // 10,
        tight=True,
    )
    gother = core_swap(gcat)
    part_list = call(
        partial_kernel,
        ids,
        [gcat, gother, wg, wu, og, ou],
        [sds((slots, blk), BF)] * NZ,
        2 * big,
    )
    parts = dict(zip(STEPS, part_list))
    parts[4] = parts[-4]

    slot_grad = ring_scatter(parts).astype(BF)
    slot_grad, all_mixed = tied(slot_grad, all_mixed)
    returned = lax.all_to_all(
        slot_grad.reshape(experts, cap, blk), "sp", 0, 0, tiled=True
    ).reshape(slots, blk)
    own_cot_late, slot_grad = tied(own_cot, slot_grad)
    other_cot = core_swap(own_cot_late)
    gg, gu, gd = call(
        weight_kernel,
        ids,
        [x_all, x_other, own_cot, other_cot, gcat, hact],
        [sds((depth, f), F32), sds((depth, f), F32), sds((f, depth), F32)],
        3 * big,
    )
    returned, gg = tied(returned, gg)
    moe_grad = dot(select, returned, 0, 0)
    mixer_cot = (cotangent.astype(F32) + moe_grad).astype(BF)

    half = tok // 2
    here = lax.dynamic_slice_in_dim(mixer_cot, c * half, half, 0)
    there = lax.dynamic_slice_in_dim(mixer_cot, (1 - c) * half, half, 0)
    got = core_swap(there)
    pair = jnp.where(
        c == 0, jnp.concatenate([here, got], axis=1), jnp.concatenate([got, here], axis=1)
    )
    m_own = ring_gather(pair)
    ms = [m_own[j] for j in STEPS]
    (cols,) = call(columns_kernel, ids, ms, [sds((experts, half, blk), BF)], big // 100, tight=True)
    out_proj, _ = tied(out_proj, cols)
    mixed_mine, mixed_theirs = call(
        mixed_kernel,
        ids,
        ms + [out_proj, other_proj],
        [sds((half, blk), F32)] * 2,
        2 * tok * depth * blk,
    )
    own_cols = lax.all_to_all(cols, "sp", 0, 0, tiled=True)
    mixed_got = core_swap(mixed_theirs)
    grad_mixed = jnp.where(
        c == 0,
        jnp.concatenate([mixed_mine, mixed_got], axis=0),
        jnp.concatenate([mixed_got, mixed_mine], axis=0),
    )
    gog = (grad_mixed * conv_out).astype(BF)
    gco = grad_mixed * out_gate.astype(F32)

    ends = neighbours(gco[:1], gco[-1:])
    own_cols, *ends = tied(own_cols, *ends)
    prev, nxt = shifted(gco, *ends)
    gci = nxt * conv_taps[0] + gco * conv_taps[1] + prev * conv_taps[2]
    grad_in_gate = (gci * values.astype(F32)).astype(BF)
    grad_values = (gci * in_gate.astype(F32)).astype(BF)

    other_cols = core_swap(own_cols)
    (grad_out_proj,) = call(
        proj_kernel,
        ids,
        [own_cols, other_cols, all_mixed],
        [sds((blk, blk), F32)],
        2 * tok * depth * blk,
        tight=True,
    )
    return gog, grad_in_gate, grad_values, grad_out_proj, gg[None], gu[None], gd[None]


def solution(mesh):
    finer = Mesh(mesh.devices.reshape(mesh.shape["sp"], NZ, 2), ("sp", "z", "c"))
    rows = P("sp", ZC)
    cols = P(None, ZC)
    in_specs = (
        rows,
        rows,
        rows,
        rows,
        cols,
        cols,
        P("sp", None),
        P("sp", None),
        P("sp", None, ZC),
        P("sp", None, ZC),
        P("sp", ZC, None),
        rows,
    )
    out_specs = (rows, rows, rows, rows, P("sp", None, ZC), P("sp", None, ZC), P("sp", ZC, None))
    return jax.shard_map(body, mesh=finer, in_specs=in_specs, out_specs=out_specs, check_vma=False)
```

```python
import functools

import jax
import jax.numpy as jnp
from jax import lax
from jax.experimental import pallas as pl
from jax.experimental.pallas import tpu as pltpu
from jax.sharding import Mesh
from jax.sharding import PartitionSpec as P


BF = jnp.bfloat16
F32 = jnp.float32
NZ = 8
ZC = ("z", "c")
STEPS = (0, -1, -2, -3, -4, 1, 2, 3)
CORE_SWAP = [(0, 1), (1, 0)]


def tied(*arrays):
    return lax.optimization_barrier(arrays)


def along(sign):
    return [(z * 2 + c, (z + sign * (1 - 2 * c)) % NZ * 2 + c) for z in range(NZ) for c in range(2)]


def ring_gather(block, note=lambda k, blocks: None):
    blocks = {0: block}
    for k in range(1, 5):
        blocks[-k] = lax.ppermute(blocks[1 - k], ZC, along(1))
        if k < 4:
            blocks[k] = lax.ppermute(blocks[k - 1], ZC, along(-1))
            blocks[-k], blocks[k] = tied(blocks[-k], blocks[k])
        note(k, blocks)
    return blocks


def core_swap(array):
    return lax.ppermute(array, "c", CORE_SWAP)


def add_rounded(a, b):
    return (a.astype(F32) + b.astype(F32)).astype(BF)


def ring_scatter(parts):
    up, down = parts[4], parts[-3]
    for k in range(3, -1, -1):
        up = lax.ppermute(up, ZC, along(1))
        if k < 3:
            down = lax.ppermute(down, ZC, along(-1))
        if k:
            up = add_rounded(up, parts[k])
            if k < 3:
                down = add_rounded(down, parts[-k])
            up, down = tied(up, down)
    return parts[0].astype(F32) + up.astype(F32) + down.astype(F32)


def block_ids():
    z, c = lax.axis_index("z"), lax.axis_index("c")
    sgn = 1 - 2 * c
    own = [(z + sgn * j + NZ) % NZ * 2 + c for j in STEPS]
    other = [(z - sgn * j + NZ) % NZ * 2 + (1 - c) for j in STEPS]
    return jnp.stack(own + other).astype(jnp.int32)


def room(args, outs):
    return sum(a.size * a.dtype.itemsize for a in (*args, *outs)) * 3 // 2 + (4 << 20)


def call(kernel, ids, args, outs, flops, tight=False):
    vmem = pl.BlockSpec(memory_space=pltpu.VMEM)
    return pl.pallas_call(
        kernel,
        in_specs=[pl.BlockSpec(memory_space=pltpu.SMEM)] + [vmem] * len(args),
        out_specs=[vmem] * len(outs),
        out_shape=outs,
        cost_estimate=pl.CostEstimate(flops=flops, bytes_accessed=flops // 500, transcendentals=0),
        compiler_params=pltpu.CompilerParams(vmem_limit_bytes=room(args, outs) if tight else None),
    )(ids, *args)


def dot(a, b, ca, cb):
    return lax.dot_general(a, b, (((ca,), (cb,)), ((), ())), preferred_element_type=F32)


def rows_of(ids, i, width):
    return pl.ds(pl.multiple_of(ids[i] * width, width), width)


def forward_kernel(ids, *refs):
    xs, (wg, wu, og, ou, mine, theirs, x_all) = refs[:NZ], refs[NZ:]
    total = None
    for i, x in enumerate(xs):
        at = rows_of(ids, i, x.shape[1])
        w = jnp.concatenate([wg[at, :], wu[at, :], og[at, :], ou[at, :]], axis=1)
        x_all[i] = x[...]
        part = dot(x[...], w, 1, 0)
        total = part if total is None else total + part
    width = mine.shape[1]
    mine[...] = total[:, :width]
    theirs[...] = total[:, width:]


def hidden_kernel(ids, cot, wd, od, fwd_theirs, mine, theirs):
    f = wd.shape[0]
    width = cot.shape[1] // NZ
    mine[...] = jnp.zeros_like(mine)
    theirs[:, : 2 * f] = fwd_theirs[...]
    theirs[:, 2 * f :] = jnp.zeros_like(mine)

    def step(j, carry):
        here = pl.ds(pl.multiple_of(j * width, width), width)
        at = rows_of(ids, j, width)
        w = jnp.concatenate([wd[:, at], od[:, at]], axis=0)
        part = dot(cot[:, here], w, 1, 1)
        mine[...] += part[:, :f]
        theirs[:, 2 * f :] += part[:, f:]
        return carry

    lax.fori_loop(0, NZ, step, 0)


def grads_kernel(ids, fmine, hmine, theirs, hact, gcat):
    f = hmine.shape[1]
    total = hmine[...] + theirs[:, 2 * f :]
    gate = fmine[:, :f] + theirs[:, :f]
    up = fmine[:, f:] + theirs[:, f : 2 * f]
    sig = jax.nn.sigmoid(gate)
    act = gate * sig
    hact[...] = (act * up).astype(BF)
    gcat[:, :f] = (total * up * sig * (1.0 + gate * (1.0 - sig))).astype(BF)
    gcat[:, f:] = (total * act).astype(BF)


def partial_kernel(ids, gcat, gother, wg, wu, og, ou, *parts):
    g = jnp.concatenate([gcat[...], gother[...]], axis=1)
    for i, part in enumerate(parts):
        at = rows_of(ids, i, part.shape[1])
        w = jnp.concatenate([wg[at, :], wu[at, :], og[at, :], ou[at, :]], axis=1)
        part[...] = dot(g, w, 1, 1).astype(BF)


def weight_kernel(ids, x_own, x_other, gcat, gg, gu):
    f = gg.shape[1]
    width = x_own.shape[2]

    def step(j, carry):
        for base, xs in ((0, x_own), (NZ, x_other)):
            both = dot(xs[j], gcat[...], 0, 0)
            at = rows_of(ids, base + j, width)
            gg[at, :] = both[:, :f]
            gu[at, :] = both[:, f:]
        return carry

    lax.fori_loop(0, NZ, step, 0)


def down_kernel(ids, own, other, hact, gd):
    width = own.shape[1] // NZ

    def step(j, carry):
        here = pl.ds(pl.multiple_of(j * width, width), width)
        for base, cot in ((0, own), (NZ, other)):
            at = rows_of(ids, base + j, width)
            gd[:, at] = dot(hact[...], cot[:, here], 0, 0)
        return carry

    lax.fori_loop(0, NZ, step, 0)


def columns_kernel(ids, *refs):
    ms, cols = refs[:NZ], refs[NZ]
    width = cols.shape[2]
    for i, m in enumerate(ms):
        for p in range(2):
            cols[ids[i] // 2 * 2 + p] = m[:, p * width : (p + 1) * width]


def mixed_kernel(ids, *refs):
    ms, (proj, other_proj, mine, theirs) = refs[:NZ], refs[NZ:]
    total = None
    for i, m in enumerate(ms):
        wide = m.shape[1]
        at = pl.ds(pl.multiple_of(ids[i] // 2 * wide, wide), wide)
        w = jnp.concatenate([proj[at, :], other_proj[at, :]], axis=1)
        part = dot(m[...], w, 1, 0)
        total = part if total is None else total + part
    width = mine.shape[1]
    mine[...] = total[:, :width]
    theirs[...] = total[:, width:]


def proj_kernel(ids, own, other, mixed, out):
    groups, half, width = own.shape

    def part(cols, at):
        rows = mixed[:, at : at + half, :]
        flat = (groups * half, width)
        return dot(cols[...].reshape(flat), rows.reshape(flat), 0, 0)

    out[...] = part(own, 0) + part(other, half)


def neighbours(first, last):
    size = lax.axis_size("sp")
    up = [(i, i + 1) for i in range(size - 1)]
    return lax.ppermute(last, "sp", up), lax.ppermute(first, "sp", [(j, i) for i, j in up])


def shifted(array, before, after):
    return jnp.concatenate([before, array[:-1]], axis=0), jnp.concatenate([array[1:], after], axis=0)


def sds(shape, dtype):
    return jax.ShapeDtypeStruct(shape, dtype)


def body(
    moe_input,
    out_gate,
    in_gate,
    values,
    conv_taps,
    out_proj,
    route_ids,
    route_gates,
    expert_gate,
    expert_up,
    expert_down,
    cotangent,
):
    tok, blk = moe_input.shape
    experts = lax.axis_size("sp")
    cap = 3 * tok // experts
    slots = experts * cap
    c = lax.axis_index("c")
    ids = block_ids()
    wg, wu, wd = expert_gate[0], expert_up[0], expert_down[0]
    depth, f = wg.shape

    cot_blocks = ring_gather(cotangent)
    cot_tokens = jnp.concatenate([cot_blocks[j] for j in STEPS], axis=1)

    ids_t = route_ids.T
    gates_t = route_gates.T
    which = jnp.arange(experts, dtype=jnp.int32)[:, None]
    hit = [ids_t[k][None, :] == which for k in range(ids_t.shape[0])]
    chosen = functools.reduce(jnp.logical_or, hit)
    weight = sum(jnp.where(h, gates_t[k][None, :], 0.0) for k, h in enumerate(hit))
    t = jnp.arange(tok, dtype=jnp.int32)
    before = (t[:, None] < t[None, :]).astype(BF)
    position = jnp.dot(chosen.astype(BF), before, preferred_element_type=F32).astype(jnp.int32)
    place = jnp.where(chosen, position, -1)
    pick = place[:, None, :] == jnp.arange(cap, dtype=jnp.int32)[None, :, None]
    select = pick.astype(BF).reshape(slots, tok)
    slot_weight = jnp.sum(jnp.where(pick, weight[:, None, :], 0.0), axis=2).reshape(slots, 1)

    send_x = jnp.dot(select, moe_input, preferred_element_type=F32).astype(BF)
    x0 = lax.all_to_all(send_x.reshape(experts, cap, blk), "sp", 0, 0, tiled=True)
    x0 = x0.reshape(slots, blk)
    send_c = (
        slot_weight * jnp.dot(select, cot_tokens, preferred_element_type=F32)
    ).astype(BF)

    og, ou, od = (core_swap(w) for w in (wg, wu, wd))
    other_proj = core_swap(out_proj)
    conv_in = in_gate.astype(F32) * values.astype(F32)
    held = {}

    def note(k, blocks):
        if k == 1:
            blocks[-1], blocks[1], held["conv_in"], held["od"] = tied(
                blocks[-1], blocks[1], conv_in, od
            )

    x_own = ring_gather(x0, note)
    send_c, x0 = tied(send_c, x0)
    own_cot = lax.all_to_all(
        send_c.reshape(experts, cap, NZ * blk), "sp", 0, 0, tiled=True
    ).reshape(slots, NZ * blk)
    conv_in, od = held["conv_in"], held["od"]
    conv_ends = neighbours(conv_in[:1], conv_in[-1:])
    own_cot, *conv_ends = tied(own_cot, *conv_ends)
    prev, nxt = shifted(conv_in, *conv_ends)
    conv_out = prev * conv_taps[0] + conv_in * conv_taps[1] + nxt * conv_taps[2]
    mixed = (out_gate.astype(F32) * conv_out).astype(BF)
    rolled = jnp.roll(mixed, -c * (tok // 2), axis=0)
    all_mixed = lax.all_to_all(
        jnp.broadcast_to(rolled[None], (experts, tok, blk)), "sp", 0, 0, tiled=True
    )

    big = 2 * slots * depth * f
    fwd_mine, fwd_theirs, x_all = call(
        forward_kernel,
        ids,
        [x_own[j] for j in STEPS] + [wg, wu, og, ou],
        [sds((slots, 2 * f), F32)] * 2 + [sds((NZ, slots, blk), BF)],
        2 * big,
    )
    x_other = core_swap(x_all)
    hid_mine, theirs = call(
        hidden_kernel,
        ids,
        [own_cot, wd, od, fwd_theirs],
        [sds((slots, f), F32), sds((slots, 3 * f), F32)],
        big,
        tight=True,
    )
    theirs = core_swap(theirs)
    theirs, x_other = tied(theirs, x_other)
    hact, gcat = call(
        grads_kernel,
        ids,
        [fwd_mine, hid_mine, theirs],
        [sds((slots, f), BF), sds((slots, 2 * f), BF)],
        big // 10,
        tight=True,
    )
    gother = core_swap(gcat)
    part_list = call(
        partial_kernel,
        ids,
        [gcat, gother, wg, wu, og, ou],
        [sds((slots, blk), BF)] * NZ,
        2 * big,
    )
    parts = dict(zip(STEPS, part_list))
    parts[4] = parts[-4]

    slot_grad = ring_scatter(parts).astype(BF)
    slot_grad, all_mixed = tied(slot_grad, all_mixed)
    returned = lax.all_to_all(
        slot_grad.reshape(experts, cap, blk), "sp", 0, 0, tiled=True
    ).reshape(slots, blk)
    own_cot_late, slot_grad = tied(own_cot, slot_grad)
    other_cot = core_swap(own_cot_late)
    gg, gu = call(
        weight_kernel,
        ids,
        [x_all, x_other, gcat],
        [sds((depth, f), F32)] * 2,
        2 * big,
    )
    returned, gg = tied(returned, gg)
    moe_grad = dot(select, returned, 0, 0)
    mixer_cot = (cotangent.astype(F32) + moe_grad).astype(BF)

    half = tok // 2
    here = lax.dynamic_slice_in_dim(mixer_cot, c * half, half, 0)
    there = lax.dynamic_slice_in_dim(mixer_cot, (1 - c) * half, half, 0)
    got = core_swap(there)
    pair = jnp.where(
        c == 0, jnp.concatenate([here, got], axis=1), jnp.concatenate([got, here], axis=1)
    )
    m_own = ring_gather(pair)
    ms = [m_own[j] for j in STEPS]
    (cols,) = call(columns_kernel, ids, ms, [sds((experts, half, blk), BF)], big // 100, tight=True)
    out_proj, _ = tied(out_proj, cols)
    mixed_mine, mixed_theirs = call(
        mixed_kernel,
        ids,
        ms + [out_proj, other_proj],
        [sds((half, blk), F32)] * 2,
        2 * tok * depth * blk,
    )
    own_cols = lax.all_to_all(cols, "sp", 0, 0, tiled=True)
    mixed_got = core_swap(mixed_theirs)
    grad_mixed = jnp.where(
        c == 0,
        jnp.concatenate([mixed_mine, mixed_got], axis=0),
        jnp.concatenate([mixed_got, mixed_mine], axis=0),
    )
    gog = (grad_mixed * conv_out).astype(BF)
    gco = grad_mixed * out_gate.astype(F32)

    ends = neighbours(gco[:1], gco[-1:])
    hact, gco = tied(hact, gco)
    (gd,) = call(down_kernel, ids, [own_cot, other_cot, hact], [sds((f, depth), F32)], big)
    own_cols, gd, *ends = tied(own_cols, gd, *ends)
    prev, nxt = shifted(gco, *ends)
    gci = nxt * conv_taps[0] + gco * conv_taps[1] + prev * conv_taps[2]
    grad_in_gate = (gci * values.astype(F32)).astype(BF)
    grad_values = (gci * in_gate.astype(F32)).astype(BF)

    other_cols = core_swap(own_cols)
    (grad_out_proj,) = call(
        proj_kernel,
        ids,
        [own_cols, other_cols, all_mixed],
        [sds((blk, blk), F32)],
        2 * tok * depth * blk,
        tight=True,
    )
    return gog, grad_in_gate, grad_values, grad_out_proj, gg[None], gu[None], gd[None]


def solution(mesh):
    finer = Mesh(mesh.devices.reshape(mesh.shape["sp"], NZ, 2), ("sp", "z", "c"))
    rows = P("sp", ZC)
    cols = P(None, ZC)
    in_specs = (
        rows,
        rows,
        rows,
        rows,
        cols,
        cols,
        P("sp", None),
        P("sp", None),
        P("sp", None, ZC),
        P("sp", None, ZC),
        P("sp", ZC, None),
        rows,
    )
    out_specs = (rows, rows, rows, rows, P("sp", None, ZC), P("sp", None, ZC), P("sp", ZC, None))
    return jax.shard_map(body, mesh=finer, in_specs=in_specs, out_specs=out_specs, check_vma=False)
```
